256 devices in a mesh: grp: 2 (over y), fs: 32 (over z, core), tp: 4 (over x).
Axes of the slice: x: 4, y: 2, z: 16, core: 2. Of those that a mesh axis runs over, the one named last changes fastest.
The devices are a block of a 4x16x16 slice.
Arguments:
- tokens: bfloat16 [1536, 2048], P(('grp', 'tp')), parts along dimension 0, may hold values from -6 to 6
- norm_gain: float32 [2048], P('fs'), may hold values from 0.1 to 1.9
- up_trained: float32 [2048, 8192], P('fs', 'tp'), may hold values from -0.125 to 0.125
- down_trained: float32 [2048, 8192], P('fs', 'tp'), may hold values from -0.125 to 0.125
Outputs:
- up_serving: bfloat16 [4096, 8192], P('grp', 'fs'), parts along dimension 0
- down_serving: bfloat16 [4096, 8192], P('grp', 'fs'), parts along dimension 0
- prompt_output: bfloat16 [1536, 2048], P(('grp', 'tp'), 'fs'), parts along dimension 0
The draws below stay inside these ranges and needn't reach their ends.
There are 2 independent parts, one for each index of `grp`. The reference program is written for one: setup_inputs(seed, part) draws one part's arguments, and reference() takes and returns one part's arrays. A program takes and returns all parts, laid end to end along the dimension named above; an argument that names none is the same for every part. Nothing has to cross between parts.
All inputs are finite; a program needn't handle non-finite values.
Results may differ from the reference program's by a relative error of at most 0.0074.
Values may be sent and summed in bfloat16 or wider, within the bound.
No kernel may reach another device: no remote copies, remote signals or barrier semaphores. Data moves between devices by JAX's collectives and lax.ppermute only.
A program may use at most 64 MiB of HBM per device.

```python
import jax
import jax.numpy as jnp
from jax import lax

D = 2048
FF = 8192
TOKENS = 768


def with_spikes(entries, stream_key, source, target, parts, factor):
    owner, partner = [(jnp.arange(entries.shape[axis_at]) // (entries.shape[axis_at] // parts)).reshape([-1 if axis == axis_at else 1 for axis in range(entries.ndim)]) for axis_at in (source, target)]
    chosen = jax.random.permutation(stream_key, parts)[partner]
    strong = (owner == chosen) | (owner == (partner + parts // 2) % parts)
    return jnp.where(strong, factor * entries, entries)


def levels(rng, extent, shards, least, top_value):
    def one(dim, blocks):
        heights = jax.random.uniform(jax.random.fold_in(jax.random.fold_in(rng, 6), dim), (blocks,), jnp.float32, least / len(shards), top_value / len(shards))
        return jnp.repeat(jnp.exp(heights), extent[dim] // blocks).reshape((-1,) + (1,) * (len(extent) - dim - 1))

    factor_of = one(*shards[0])
    for cut in shards[1:]:
        factor_of = factor_of * one(*cut)
    return factor_of


def normal_values(rng, shape, spread, most, shards=(), dtype=jnp.bfloat16):
    entries = jax.random.normal(rng, shape, jnp.float32) * spread
    if len(shards) > 0:
        entries = levels(rng, shape, shards, -0.22, 0.18) * entries
    return jnp.clip(entries, min=-most, max=most).astype(dtype)


def bell_draw_with(stream_key, extent, scale, reach, cuts, heavy, kind=jnp.bfloat16):
    entries = scale * jax.random.normal(stream_key, extent, jnp.float32)
    if cuts:
        entries = entries * levels(stream_key, extent, cuts, -0.22, 0.18)
    return jnp.clip(with_spikes(entries, jax.random.fold_in(stream_key, 3), *heavy), -reach, reach).astype(kind)


def setup_inputs(seed: int = 0, part: int = 0) -> dict:
    streams_of = jax.random.split(jax.random.key(seed), 5)
    own_keys = jax.random.split(jax.random.fold_in(streams_of[4], part), 5)
    return {
        "tokens": normal_values(own_keys[0], (TOKENS, D), 1.0, 6.0, ((0, 4),)),
        "norm_gain": jnp.clip(1.0 + 0.18 * jax.random.normal(streams_of[1], (D,), jnp.float32), 0.1, 1.9),
        "up_trained": normal_values(streams_of[2], (D, FF), D ** -0.5, 0.125, ((0, 32), (1, 4)), jnp.float32),
        "down_trained": bell_draw_with(streams_of[3], (D, FF), FF ** -0.5, 0.125, ((0, 32), (1, 4)), (1, 0, 32, 2.75), jnp.float32),
    }


epsilon = 1e-06

def reference(tokens, norm_gain, up_trained, down_trained):
    up_serving = (norm_gain[:, None] * up_trained).astype(jnp.bfloat16)
    down_serving = down_trained.astype(jnp.bfloat16)
    values = tokens.astype(jnp.float32)
    scale = lax.rsqrt(lax.optimization_barrier(jnp.mean(values * values, axis=1, keepdims=True)) + epsilon)
    normed = (values * scale).astype(jnp.bfloat16)
    hidden = jnp.dot(normed, up_serving, preferred_element_type=jnp.float32)
    active = jnp.square(jax.nn.relu(hidden)).astype(jnp.bfloat16)
    prompt_output = jnp.dot(active, down_serving.T, preferred_element_type=jnp.float32).astype(jnp.bfloat16)
    return (up_serving, down_serving, prompt_output)
```

```python
import jax
import jax.numpy as jnp
from jax import lax
from jax.sharding import PartitionSpec as P

epsilon = 1e-06
CORES = 2


def joined_along(parts, dim):
    parts = jnp.moveaxis(parts, 0, dim)
    dims = parts.shape
    return parts.reshape(*dims[:dim], dims[dim] * dims[dim + 1], *dims[dim + 2 :])


def copy_for_each(x, axis):
    devices = lax.axis_size(axis)
    return lax.all_to_all(jnp.broadcast_to(x[None], (devices, *x.shape)), axis, 0, 0, tiled=True)


def collect(x, axis, dim):
    return joined_along(copy_for_each(x, axis), dim)


def packed(x):
    rows, cols = x.shape[-2:]
    wide = cols * 2 // 3
    tail = x[..., wide:]
    tail = jnp.concatenate([tail[..., : rows // 2, :], tail[..., rows // 2 :, :]], axis=-1)
    return jnp.concatenate([x[..., :wide], tail], axis=-2)


def unpacked(x, rows):
    wide = x.shape[-1]
    tail = x[..., rows:, :]
    tail = jnp.concatenate([tail[..., : wide // 2], tail[..., wide // 2 :]], axis=-2)
    return jnp.concatenate([x[..., :rows, :], tail], axis=-1)


def sum_at_owner(x, axis):
    devices = lax.axis_size(axis)
    rows = x.shape[0] // devices
    chips = devices // CORES
    parts = packed(x.reshape(chips, CORES, rows, x.shape[1]))
    core = lax.axis_index(axis) % CORES
    away = lax.dynamic_index_in_dim(parts, 1 - core, 1, keepdims=False)
    kept = lax.dynamic_index_in_dim(parts, core, 1, keepdims=False)
    other = lax.ppermute(away, axis, [(i, i ^ 1) for i in range(devices)])
    both = (kept.astype(jnp.float32) + other.astype(jnp.float32)).astype(jnp.bfloat16)
    same_core = [[z * CORES + c for z in range(chips)] for c in range(CORES)]
    arrived = lax.all_to_all(both, axis, 0, 0, axis_index_groups=same_core, tiled=True)
    return unpacked(arrived.astype(jnp.float32).sum(axis=0), rows)


def local(tokens, norm_gain, up_trained, down_trained):
    shards = lax.axis_size("fs")
    groups = lax.axis_size("tp")
    rows_local = up_trained.shape[0]
    cols_local = up_trained.shape[1]
    folded = (norm_gain[:, None] * up_trained).astype(jnp.bfloat16)
    stacked = jnp.stack([folded, down_trained.astype(jnp.bfloat16)])
    served_width = cols_local * groups // shards
    blocks_here = cols_local // served_width
    quarter_rows = rows_local // groups
    pieces = stacked.reshape(2, groups, quarter_rows, blocks_here, served_width)
    moved = lax.all_to_all(pieces, "tp", split_axis=1, concat_axis=3, tiled=True)
    placed = lax.all_to_all(moved, "fs", split_axis=3, concat_axis=2, tiled=True)
    ordered = placed.reshape(2, shards, quarter_rows, served_width)
    joined = collect(ordered, "tp", 2)
    owned = joined.reshape(2, rows_local * shards, served_width)
    up_serving = owned[0]
    down_serving = owned[1]
    values = tokens.astype(jnp.float32)
    scale = lax.rsqrt(jnp.mean(values * values, axis=1, keepdims=True) + epsilon)
    normed = (values * scale).astype(jnp.bfloat16)
    hidden = jnp.dot(normed, up_serving, preferred_element_type=jnp.float32)
    active = jnp.square(jax.nn.relu(hidden)).astype(jnp.bfloat16)
    partial = lax.dot_general(
        down_serving, active, (((1,), (1,)), ((), ())), preferred_element_type=jnp.float32
    ).astype(jnp.bfloat16)
    prompt_output = sum_at_owner(partial, "fs").T.astype(jnp.bfloat16)
    return (up_serving, down_serving, prompt_output)


def solution(mesh):
    in_specs = (P(("grp", "tp"), None), P("fs"), P("fs", "tp"), P("fs", "tp"))
    out_specs = (P("grp", "fs"), P("grp", "fs"), P(("grp", "tp"), "fs"))
    return jax.shard_map(local, mesh=mesh, in_specs=in_specs, out_specs=out_specs, check_vma=False)
```

```python
import functools

import jax
import jax.numpy as jnp
from jax import lax
from jax.experimental import pallas as pl
from jax.experimental.pallas import tpu as pltpu
from jax.sharding import PartitionSpec as P

epsilon = 1e-06
CORES = 2
LANES = 128


def ring(devices, step):
    return [(i, (i + step) % devices) for i in range(devices)]


def nt_dot(a, b):
    return lax.dot_general(a, b, (((1,), (1,)), ((), ())), preferred_element_type=jnp.float32)


def feed_forward(
    where, normed, own, left, right, far_up, far_down, up_out, down_out, kept, away, up, down, sems
):
    shards, groups, quarter, width = up.shape
    at, core = where[0], where[1]
    for step, (piece_up, piece_down) in enumerate(
        [(own.at[0], own.at[1]), (left.at[0], left.at[1]), (far_up, far_down), (right.at[0], right.at[1])]
    ):
        slot = lax.rem(at + step, groups)
        up[:, pl.ds(slot, 1)] = piece_up[...][:, None]
        down[:, pl.ds(slot, 1)] = piece_down[...][:, None]
    writes = [pltpu.make_async_copy(up, up_out, sems.at[0]), pltpu.make_async_copy(down, down_out, sems.at[1])]
    for write in writes:
        write.start()
    hidden = jnp.dot(
        normed[...], up[...].reshape(shards * groups * quarter, width), preferred_element_type=jnp.float32
    )
    active = jnp.square(jnp.maximum(hidden, 0.0)).astype(jnp.bfloat16)
    head, tail = active[:LANES], active[LANES:]
    none = jnp.zeros_like(tail)
    upper, lower = jnp.concatenate([tail, none]), jnp.concatenate([none, tail])
    rows, chips = groups * quarter, shards // CORES
    for out, side in ((away, 1 - core), (kept, core)):
        weights = down.reshape(chips, CORES, rows, width)[:, pl.ds(side, 1)][:, 0]
        out[:, :rows] = nt_dot(weights.reshape(chips * rows, width), head).astype(out.dtype).reshape(chips, rows, LANES)
        both = nt_dot(weights[:, : rows // 2].reshape(chips * rows // 2, width), upper) + nt_dot(
            weights[:, rows // 2 :].reshape(chips * rows // 2, width), lower
        )
        out[:, rows:] = both.astype(out.dtype).reshape(chips, rows // 2, LANES)
    for write in writes:
        write.wait()


def unpacked(x, rows):
    tail = x[rows:]
    tail = jnp.concatenate([tail[:, : LANES // 2], tail[:, LANES // 2 :]], axis=0)
    return jnp.concatenate([x[:rows], tail], axis=1)


def local(tokens, norm_gain, up_trained, down_trained):
    shards = lax.axis_size("fs")
    groups = lax.axis_size("tp")
    chips = shards // CORES
    rows_local, cols_local = up_trained.shape
    count, features = tokens.shape
    folded = (norm_gain[:, None] * up_trained).astype(jnp.bfloat16)
    stacked = jnp.stack([folded, down_trained.astype(jnp.bfloat16)])
    width = cols_local * groups // shards
    blocks_here = cols_local // width
    quarter = rows_local // groups
    pieces = stacked.reshape(2, groups, quarter, blocks_here, width)
    moved = lax.all_to_all(pieces, "tp", split_axis=1, concat_axis=3, tiled=True)
    placed = lax.all_to_all(moved, "fs", split_axis=3, concat_axis=2, tiled=True)
    own = placed.reshape(2, shards, quarter, width)
    right = lax.ppermute(own, "tp", ring(groups, 1))
    left = lax.ppermute(own, "tp", ring(groups, -1))
    far_up = lax.ppermute(right[0], "tp", ring(groups, 1))
    far_down = lax.ppermute(left[1], "tp", ring(groups, -1))
    values = tokens.astype(jnp.float32)
    scale = lax.rsqrt(jnp.mean(values * values, axis=1, keepdims=True) + epsilon)
    normed = (values * scale).astype(jnp.bfloat16)
    where = jnp.stack([lax.axis_index("tp"), lax.axis_index("fs") % CORES]).astype(jnp.int32)
    served = (shards, groups, quarter, width)
    packed_rows = rows_local * count // LANES
    vmem = pl.BlockSpec(memory_space=pltpu.VMEM)
    up_serving, down_serving, kept, away = pl.pallas_call(
        feed_forward,
        out_shape=[
            jax.ShapeDtypeStruct(served, jnp.bfloat16),
            jax.ShapeDtypeStruct(served, jnp.bfloat16),
            jax.ShapeDtypeStruct((chips, packed_rows, LANES), jnp.bfloat16),
            jax.ShapeDtypeStruct((chips, packed_rows, LANES), jnp.bfloat16),
        ],
        in_specs=[pl.BlockSpec(memory_space=pltpu.SMEM)] + [vmem] * 6,
        out_specs=[pl.BlockSpec(memory_space=pl.ANY)] * 2 + [vmem] * 2,
        scratch_shapes=[
            pltpu.VMEM(served, jnp.bfloat16),
            pltpu.VMEM(served, jnp.bfloat16),
            pltpu.SemaphoreType.DMA((2,)),
        ],
        compiler_params=pltpu.CompilerParams(vmem_limit_bytes=32 << 20),
        cost_estimate=pl.CostEstimate(
            flops=4 * count * features * width, bytes_accessed=4 * features * width * 2, transcendentals=0
        ),
        name="feed_forward",
    )(where, normed, own, left, right, far_up, far_down)
    other = lax.ppermute(away, "fs", [(i, i ^ 1) for i in range(shards)])
    summed = (kept.astype(jnp.float32) + other.astype(jnp.float32)).astype(jnp.bfloat16)
    same_core = [[z * CORES + c for z in range(chips)] for c in range(CORES)]
    arrived = lax.all_to_all(summed, "fs", 0, 0, axis_index_groups=same_core, tiled=True)
    out = unpacked(arrived.astype(jnp.float32).sum(axis=0), rows_local).T.astype(jnp.bfloat16)
    return (up_serving.reshape(features, width), down_serving.reshape(features, width), out)


def solution(mesh):
    in_specs = (P(("grp", "tp"), None), P("fs"), P("fs", "tp"), P("fs", "tp"))
    out_specs = (P("grp", "fs"), P("grp", "fs"), P(("grp", "tp"), "fs"))
    return jax.shard_map(local, mesh=mesh, in_specs=in_specs, out_specs=out_specs, check_vma=False)
```

```python
import functools

import jax
import jax.numpy as jnp
from jax import lax
from jax.experimental import pallas as pl
from jax.experimental.pallas import tpu as pltpu
from jax.sharding import PartitionSpec as P

epsilon = 1e-06
CORES = 2
LANES = 128


def ring(devices, step):
    return [(i, (i + step) % devices) for i in range(devices)]


def nt_dot(a, b):
    return lax.dot_general(a, b, (((1,), (1,)), ((), ())), preferred_element_type=jnp.float32)


def feed_forward(
    cores, where, normed, own, left, right, far_up, far_down, up_out, down_out, kept, away, up, down, sems
):
    shards, groups, quarter, width = up.shape
    at, core = where[0], where[1]
    for step, (piece_up, piece_down) in enumerate(
        [(own.at[0], own.at[1]), (left.at[0], left.at[1]), (far_up, far_down), (right.at[0], right.at[1])]
    ):
        slot = lax.rem(at + step, groups)
        up[:, pl.ds(slot, 1)] = piece_up[...][:, None]
        down[:, pl.ds(slot, 1)] = piece_down[...][:, None]
    writes = [pltpu.make_async_copy(up, up_out, sems.at[0]), pltpu.make_async_copy(down, down_out, sems.at[1])]
    for write in writes:
        write.start()
    hidden = jnp.dot(
        normed[...], up[...].reshape(shards * groups * quarter, width), preferred_element_type=jnp.float32
    )
    active = jnp.square(jnp.maximum(hidden, 0.0)).astype(jnp.bfloat16)
    head, tail = active[:LANES], active[LANES:]
    none = jnp.zeros_like(tail)
    upper, lower = jnp.concatenate([tail, none]), jnp.concatenate([none, tail])
    rows, chips = groups * quarter, shards // cores
    for out, side in ((away, 1 - core), (kept, core)):
        weights = down.reshape(chips, cores, rows, width)[:, pl.ds(side, 1)][:, 0]
        out[:, :rows] = nt_dot(weights.reshape(chips * rows, width), head).astype(out.dtype).reshape(chips, rows, LANES)
        both = nt_dot(weights[:, : rows // 2].reshape(chips * rows // 2, width), upper) + nt_dot(
            weights[:, rows // 2 :].reshape(chips * rows // 2, width), lower
        )
        out[:, rows:] = both.astype(out.dtype).reshape(chips, rows // 2, LANES)
    for write in writes:
        write.wait()


def unpacked(x, rows):
    tail = x[rows:]
    tail = jnp.concatenate([tail[:, : LANES // 2], tail[:, LANES // 2 :]], axis=0)
    return jnp.concatenate([x[:rows], tail], axis=1)


def local(tokens, norm_gain, up_trained, down_trained):
    chips, cores, groups = lax.axis_size("z"), lax.axis_size("core"), lax.axis_size("tp")
    shards = chips * cores
    rows_local, cols_local = up_trained.shape
    count, features = tokens.shape
    width = cols_local * groups // shards
    blocks = cols_local // (width * cores)
    quarter = rows_local // groups
    folded = (norm_gain[:, None] * up_trained).astype(jnp.bfloat16)
    stacked = jnp.stack([folded, down_trained.astype(jnp.bfloat16)])
    pieces = stacked.reshape(2, groups, quarter, blocks, cores, width).transpose(4, 1, 3, 0, 2, 5)
    pieces = pieces.reshape(cores * groups, blocks, 2, quarter, width)
    moved = lax.all_to_all(pieces, ("core", "tp"), 0, 0, tiled=True)
    moved = moved.reshape(cores, chips, 2, quarter, width).transpose(1, 2, 0, 3, 4)
    own = lax.all_to_all(moved, "z", 0, 0, tiled=True)
    own = own.transpose(1, 0, 2, 3, 4).reshape(2, shards, quarter, width)
    right = lax.ppermute(own, "tp", ring(groups, 1))
    left = lax.ppermute(own, "tp", ring(groups, -1))
    far_up = lax.ppermute(right[0], "tp", ring(groups, 1))
    far_down = lax.ppermute(left[1], "tp", ring(groups, -1))
    values = tokens.astype(jnp.float32)
    scale = lax.rsqrt(jnp.mean(values * values, axis=1, keepdims=True) + epsilon)
    normed = (values * scale).astype(jnp.bfloat16)
    where = jnp.stack([lax.axis_index("tp"), lax.axis_index("core")]).astype(jnp.int32)
    served = (shards, groups, quarter, width)
    packed_rows = rows_local * count // LANES
    vmem = pl.BlockSpec(memory_space=pltpu.VMEM)
    up_serving, down_serving, kept, away = pl.pallas_call(
        functools.partial(feed_forward, cores),
        out_shape=[
            jax.ShapeDtypeStruct(served, jnp.bfloat16),
            jax.ShapeDtypeStruct(served, jnp.bfloat16),
            jax.ShapeDtypeStruct((chips, packed_rows, LANES), jnp.bfloat16),
            jax.ShapeDtypeStruct((chips, packed_rows, LANES), jnp.bfloat16),
        ],
        in_specs=[pl.BlockSpec(memory_space=pltpu.SMEM)] + [vmem] * 6,
        out_specs=[pl.BlockSpec(memory_space=pl.ANY)] * 2 + [vmem] * 2,
        scratch_shapes=[
            pltpu.VMEM(served, jnp.bfloat16),
            pltpu.VMEM(served, jnp.bfloat16),
            pltpu.SemaphoreType.DMA((2,)),
        ],
        compiler_params=pltpu.CompilerParams(vmem_limit_bytes=32 << 20),
        cost_estimate=pl.CostEstimate(
            flops=4 * count * features * width, bytes_accessed=4 * features * width * 2, transcendentals=0
        ),
        name="feed_forward",
    )(where, normed, own, left, right, far_up, far_down)
    other = lax.ppermute(away, "core", ring(cores, 1))
    summed = (kept.astype(jnp.float32) + other.astype(jnp.float32)).astype(jnp.bfloat16)
    arrived = lax.all_to_all(summed, "z", 0, 0, tiled=True)
    out = unpacked(arrived.astype(jnp.float32).sum(axis=0), rows_local).T.astype(jnp.bfloat16)
    return (up_serving.reshape(features, width), down_serving.reshape(features, width), out)


def solution(mesh):
    sizes = mesh.shape
    devices = mesh.devices.reshape(sizes["grp"], sizes["fs"] // CORES, CORES, sizes["tp"])
    mesh = jax.sharding.Mesh(devices, ("grp", "z", "core", "tp"))
    fs = ("z", "core")
    in_specs = (P(("grp", "tp"), None), P(fs), P(fs, "tp"), P(fs, "tp"))
    out_specs = (P("grp", fs), P("grp", fs), P(("grp", "tp"), fs))
    return jax.shard_map(local, mesh=mesh, in_specs=in_specs, out_specs=out_specs, check_vma=False)
```

```python
import functools

import jax
import jax.numpy as jnp
from jax import lax
from jax.experimental import pallas as pl
from jax.experimental.pallas import tpu as pltpu
from jax.sharding import PartitionSpec as P

epsilon = 1e-06
CORES = 2
PAIR = 2
LANES = 128


def ring(devices, step):
    return [(i, (i + step) % devices) for i in range(devices)]


def across(devices, step):
    return [
        (member * devices + i, (1 - member) * devices + (i + step) % devices)
        for member in range(PAIR)
        for i in range(devices)
    ]


def nt_dot(a, b):
    return lax.dot_general(a, b, (((1,), (1,)), ((), ())), preferred_element_type=jnp.float32)


def feed_forward(cores, where, normed, *refs):
    quarters, (up_out, down_out, kept, away, both, sems) = refs[:-6], refs[-6:]
    _, shards, groups, quarter, width = both.shape
    at, core, member = where[0], where[1], where[2]
    for weight, (own, left, far_first, far_second, right) in (
        (member, quarters[:5]),
        (1 - member, quarters[5:]),
    ):
        half = shards // 2
        for step, first, count, piece in (
            (0, 0, shards, own),
            (1, 0, shards, left),
            (2, 0, half, far_first),
            (2, half, half, far_second),
            (3, 0, shards, right),
        ):
            slot = lax.rem(at + step, groups)
            both[pl.ds(weight, 1), pl.ds(first, count), pl.ds(slot, 1)] = piece[...][None, :, None]
    writes = [
        pltpu.make_async_copy(both.at[0], up_out, sems.at[0]),
        pltpu.make_async_copy(both.at[1], down_out, sems.at[1]),
    ]
    hidden = jnp.dot(
        normed[...], both[0].reshape(shards * groups * quarter, width), preferred_element_type=jnp.float32
    )
    active = jnp.square(jnp.maximum(hidden, 0.0)).astype(jnp.bfloat16)
    for write in writes:
        write.start()
    head, tail = active[:LANES], active[LANES:]
    none = jnp.zeros_like(tail)
    upper, lower = jnp.concatenate([tail, none]), jnp.concatenate([none, tail])
    rows, chips = groups * quarter, shards // cores
    down = both.at[1].reshape(chips, cores, rows, width)
    for out, side in ((away, 1 - core), (kept, core)):
        weights = down[:, pl.ds(side, 1)][:, 0]
        out[:, :rows] = nt_dot(weights.reshape(chips * rows, width), head).astype(out.dtype).reshape(chips, rows, LANES)
        packed = nt_dot(weights[:, : rows // 2].reshape(chips * rows // 2, width), upper) + nt_dot(
            weights[:, rows // 2 :].reshape(chips * rows // 2, width), lower
        )
        out[:, rows:] = packed.astype(out.dtype).reshape(chips, rows // 2, LANES)
    for write in writes:
        write.wait()


def unpacked(x, rows):
    tail = x[rows:]
    tail = jnp.concatenate([tail[:, : LANES // 2], tail[:, LANES // 2 :]], axis=0)
    return jnp.concatenate([x[:rows], tail], axis=1)


def local(tokens, norm_gain, up_trained, down_trained):
    chips, cores, groups = lax.axis_size("z"), lax.axis_size("core"), lax.axis_size("tp")
    member = lax.axis_index("member")
    shards = chips * cores
    rows_local, cols_local = up_trained.shape
    count, features = tokens.shape
    width = cols_local * groups // shards
    blocks = cols_local // (width * cores)
    quarter = rows_local // groups
    mine = jnp.where(member == 0, norm_gain[:, None] * up_trained, down_trained).astype(jnp.bfloat16)
    pieces = mine.reshape(groups, quarter, blocks, cores, width).transpose(3, 0, 2, 1, 4)
    pieces = pieces.reshape(cores * groups, blocks, quarter, width)
    moved = lax.all_to_all(pieces, ("core", "tp"), 0, 0, tiled=True)
    moved = moved.reshape(cores, chips, quarter, width).transpose(1, 0, 2, 3)
    own = lax.all_to_all(moved, "z", 0, 0, tiled=True).reshape(shards, quarter, width)
    half = shards // 2
    right = lax.ppermute(own, "tp", ring(groups, 1))
    left = lax.ppermute(own, "tp", ring(groups, -1))
    twin = lax.ppermute(own, "member", ring(PAIR, 1))
    twin_right = lax.ppermute(twin, "tp", ring(groups, 1))
    twin_left = lax.ppermute(twin, "tp", ring(groups, -1))
    far_first = lax.ppermute(right[:half], "tp", ring(groups, 1))
    far_second = lax.ppermute(left[half:], "tp", ring(groups, -1))
    twin_far_first = lax.ppermute(left[:half], ("member", "tp"), across(groups, -1))
    twin_far_second = lax.ppermute(right[half:], ("member", "tp"), across(groups, 1))
    values = tokens.astype(jnp.float32)
    scale = lax.rsqrt(jnp.mean(values * values, axis=1, keepdims=True) + epsilon)
    normed = (values * scale).astype(jnp.bfloat16)
    where = jnp.stack([lax.axis_index("tp"), lax.axis_index("core"), member]).astype(jnp.int32)
    served = (shards, groups, quarter, width)
    packed_rows = rows_local * count // LANES
    vmem = pl.BlockSpec(memory_space=pltpu.VMEM)
    up_serving, down_serving, kept, away = pl.pallas_call(
        functools.partial(feed_forward, cores),
        out_shape=[
            jax.ShapeDtypeStruct(served, jnp.bfloat16),
            jax.ShapeDtypeStruct(served, jnp.bfloat16),
            jax.ShapeDtypeStruct((chips, packed_rows, LANES), jnp.bfloat16),
            jax.ShapeDtypeStruct((chips, packed_rows, LANES), jnp.bfloat16),
        ],
        in_specs=[pl.BlockSpec(memory_space=pltpu.SMEM)] + [vmem] * 11,
        out_specs=[pl.BlockSpec(memory_space=pl.ANY)] * 2 + [vmem] * 2,
        scratch_shapes=[
            pltpu.VMEM((2, *served), jnp.bfloat16),
            pltpu.SemaphoreType.DMA((2,)),
        ],
        compiler_params=pltpu.CompilerParams(vmem_limit_bytes=32 << 20),
        cost_estimate=pl.CostEstimate(
            flops=4 * count * features * width, bytes_accessed=4 * features * width * 2, transcendentals=0
        ),
        name="feed_forward",
    )(
        where, normed, own, left, far_first, far_second, right,
        twin, twin_left, twin_far_first, twin_far_second, twin_right,
    )
    other = lax.ppermute(away, "core", ring(cores, 1))
    summed = (kept.astype(jnp.float32) + other.astype(jnp.float32)).astype(jnp.bfloat16)
    arrived = lax.all_to_all(summed, "z", 0, 0, tiled=True)
    out = unpacked(arrived.astype(jnp.float32).sum(axis=0), rows_local).T.astype(jnp.bfloat16)
    return (up_serving.reshape(features, width), down_serving.reshape(features, width), out)


def solution(mesh):
    sizes = mesh.shape
    devices = mesh.devices.reshape(sizes["grp"] // PAIR, PAIR, sizes["fs"] // CORES, CORES, sizes["tp"])
    mesh = jax.sharding.Mesh(devices, ("pair", "member", "z", "core", "tp"))
    grp, fs = ("pair", "member"), ("z", "core")
    in_specs = (P((*grp, "tp"), None), P(fs), P(fs, "tp"), P(fs, "tp"))
    out_specs = (P(grp, fs), P(grp, fs), P((*grp, "tp"), fs))
    return jax.shard_map(local, mesh=mesh, in_specs=in_specs, out_specs=out_specs, check_vma=False)
```

```python
import functools

import jax
import jax.numpy as jnp
from jax import lax
from jax.experimental import pallas as pl
from jax.experimental.pallas import tpu as pltpu
from jax.sharding import PartitionSpec as P

epsilon = 1e-06
CORES = 2
PAIR = 2
LANES = 128


def ring(devices, step):
    return [(i, (i + step) % devices) for i in range(devices)]


def across(devices, step):
    return [
        (member * devices + i, (1 - member) * devices + (i + step) % devices)
        for member in range(PAIR)
        for i in range(devices)
    ]


def nt_dot(a, b):
    return lax.dot_general(a, b, (((1,), (1,)), ((), ())), preferred_element_type=jnp.float32)


def partial_sums(out, parity, side, cores, active, down):
    shards, groups, quarter, width = down.shape
    rows, blocks = groups * quarter, shards // cores // 2
    head, tail = active[:LANES], active[LANES:]
    none = jnp.zeros_like(tail)
    upper, lower = jnp.concatenate([tail, none]), jnp.concatenate([none, tail])
    for part in (1, 0):
        on = lax.rem(parity + part, 2) * cores + side
        weights = down.reshape(blocks, 2 * cores, rows, width)[:, pl.ds(on, 1)][:, 0]
        wide = nt_dot(weights.reshape(blocks * rows, width), head)
        out[part, :, :rows] = wide.astype(out.dtype).reshape(blocks, rows, LANES)
        packed = nt_dot(weights[:, : rows // 2].reshape(blocks * rows // 2, width), upper) + nt_dot(
            weights[:, rows // 2 :].reshape(blocks * rows // 2, width), lower
        )
        out[part, :, rows:] = packed.astype(out.dtype).reshape(blocks, rows // 2, LANES)


def feed_forward(cores, where, normed, *refs):
    quarters, (up, down, active, away) = refs[:-4], refs[-4:]
    shards, groups, quarter, width = up.shape
    at, core, member, parity = where[0], where[1], where[2], where[3]

    def place(weight, own, left, far_first, far_second, right):
        half = shards // 2
        for step, first, count, piece in (
            (0, 0, shards, own),
            (1, 0, shards, left),
            (2, 0, half, far_first),
            (2, half, half, far_second),
            (3, 0, shards, right),
        ):
            slot = lax.rem(at + step, groups)
            weight[pl.ds(first, count), pl.ds(slot, 1)] = piece[...][:, None]

    for value, mine, other in ((0, up, down), (1, down, up)):

        @pl.when(member == value)
        def _(mine=mine, other=other):
            place(mine, *quarters[:5])
            place(other, *quarters[5:])

    hidden = jnp.dot(
        normed[...], up[...].reshape(shards * groups * quarter, width), preferred_element_type=jnp.float32
    )
    rounded = jnp.square(jnp.maximum(hidden, 0.0)).astype(active.dtype)
    active[...] = rounded
    partial_sums(away, parity, 1 - core, cores, rounded, down)


def own_side(cores, where, active, up, down, up_out, down_out, kept, sems):
    writes = [pltpu.make_async_copy(up, up_out, sems.at[0]), pltpu.make_async_copy(down, down_out, sems.at[1])]
    for write in writes:
        write.start()
    partial_sums(kept, where[3], where[1], cores, active[...], down)
    for write in writes:
        write.wait()


def added(a, b):
    return (a.astype(jnp.float32) + b.astype(jnp.float32)).astype(jnp.bfloat16)


def unpacked(x, rows):
    tail = x[rows:]
    tail = jnp.concatenate([tail[:, : LANES // 2], tail[:, LANES // 2 :]], axis=0)
    return jnp.concatenate([x[:rows], tail], axis=1)


def local(tokens, norm_gain, up_trained, down_trained):
    chips, cores, groups = lax.axis_size("z"), lax.axis_size("core"), lax.axis_size("tp")
    member = lax.axis_index("member")
    shards = chips * cores
    rows_local, cols_local = up_trained.shape
    count, features = tokens.shape
    width = cols_local * groups // shards
    blocks = cols_local // (width * cores)
    quarter = rows_local // groups
    mine = jnp.where(member == 0, norm_gain[:, None] * up_trained, down_trained).astype(jnp.bfloat16)
    pieces = mine.reshape(groups, quarter, blocks, cores, width).transpose(3, 0, 2, 1, 4)
    pieces = pieces.reshape(cores * groups, blocks, quarter, width)
    moved = lax.all_to_all(pieces, ("core", "tp"), 0, 0, tiled=True)
    moved = moved.reshape(cores, chips, quarter, width).transpose(1, 0, 2, 3)
    own = lax.all_to_all(moved, "z", 0, 0, tiled=True).reshape(shards, quarter, width)
    half = shards // 2
    right = lax.ppermute(own, "tp", ring(groups, 1))
    left = lax.ppermute(own, "tp", ring(groups, -1))
    twin = lax.ppermute(own, "member", ring(PAIR, 1))
    twin_right = lax.ppermute(twin, "tp", ring(groups, 1))
    twin_left = lax.ppermute(twin, "tp", ring(groups, -1))
    far_first = lax.ppermute(right[:half], "tp", ring(groups, 1))
    far_second = lax.ppermute(left[half:], "tp", ring(groups, -1))
    twin_far_first = lax.ppermute(left[:half], ("member", "tp"), across(groups, -1))
    twin_far_second = lax.ppermute(right[half:], ("member", "tp"), across(groups, 1))
    values = tokens.astype(jnp.float32)
    scale = lax.rsqrt(jnp.mean(values * values, axis=1, keepdims=True) + epsilon)
    normed = (values * scale).astype(jnp.bfloat16)
    parity = lax.axis_index("z") % 2
    where = jnp.stack([lax.axis_index("tp"), lax.axis_index("core"), member, parity]).astype(jnp.int32)
    served = jax.ShapeDtypeStruct((shards, groups, quarter, width), jnp.bfloat16)
    part = jax.ShapeDtypeStruct((2, chips // 2, rows_local * count // LANES, LANES), jnp.bfloat16)
    smem, vmem = pl.BlockSpec(memory_space=pltpu.SMEM), pl.BlockSpec(memory_space=pltpu.VMEM)
    up, down, active, away = pl.pallas_call(
        functools.partial(feed_forward, cores),
        out_shape=[served, served, jax.ShapeDtypeStruct((count, width), jnp.bfloat16), part],
        in_specs=[smem] + [vmem] * 11,
        out_specs=[vmem] * 4,
        compiler_params=pltpu.CompilerParams(vmem_limit_bytes=24 << 20),
        cost_estimate=pl.CostEstimate(
            flops=3 * count * features * width, bytes_accessed=8 * features * width, transcendentals=0
        ),
        name="feed_forward",
    )(
        where, normed, own, left, far_first, far_second, right,
        twin, twin_left, twin_far_first, twin_far_second, twin_right,
    )
    up_serving, down_serving, kept = pl.pallas_call(
        functools.partial(own_side, cores),
        out_shape=[served, served, part],
        in_specs=[smem] + [vmem] * 3,
        out_specs=[pl.BlockSpec(memory_space=pl.ANY)] * 2 + [vmem],
        scratch_shapes=[pltpu.SemaphoreType.DMA((2,))],
        compiler_params=pltpu.CompilerParams(vmem_limit_bytes=16 << 20),
        cost_estimate=pl.CostEstimate(
            flops=count * features * width, bytes_accessed=8 * features * width, transcendentals=0
        ),
        name="own_side",
    )(where, active, up, down)
    swapped = lax.ppermute(away, "core", ring(cores, 1))
    leaving = added(kept[1], swapped[1])
    beside = lax.ppermute(leaving, "z", [(i, i ^ 1) for i in range(chips)])
    summed = added(added(kept[0], swapped[0]), beside)
    same_parity = [list(range(first, chips, 2)) for first in range(2)]
    arrived = lax.all_to_all(summed, "z", 0, 0, axis_index_groups=same_parity, tiled=True)
    out = unpacked(arrived.astype(jnp.float32).sum(axis=0), rows_local).T.astype(jnp.bfloat16)
    return (up_serving.reshape(features, width), down_serving.reshape(features, width), out)


def solution(mesh):
    sizes = mesh.shape
    devices = mesh.devices.reshape(sizes["grp"] // PAIR, PAIR, sizes["fs"] // CORES, CORES, sizes["tp"])
    mesh = jax.sharding.Mesh(devices, ("pair", "member", "z", "core", "tp"))
    grp, fs = ("pair", "member"), ("z", "core")
    in_specs = (P((*grp, "tp"), None), P(fs), P(fs, "tp"), P(fs, "tp"))
    out_specs = (P(grp, fs), P(grp, fs), P((*grp, "tp"), fs))
    return jax.shard_map(local, mesh=mesh, in_specs=in_specs, out_specs=out_specs, check_vma=False)
```

```python
import functools

import jax
import jax.numpy as jnp
from jax import lax
from jax.experimental import pallas as pl
from jax.experimental.pallas import tpu as pltpu
from jax.sharding import PartitionSpec as P


epsilon = 1e-06
CORES = 2
PAIR = 2
LANES = 128


def ring(devices, step):
    return [(i, (i + step) % devices) for i in range(devices)]


def across(devices, step):
    return [
        (member * devices + i, (1 - member) * devices + (i + step) % devices)
        for member in range(PAIR)
        for i in range(devices)
    ]


def nt_dot(a, b):
    return lax.dot_general(a, b, (((1,), (1,)), ((), ())), preferred_element_type=jnp.float32)


def partial_sums(out, side, cores, active, down):
    shards, groups, quarter, width = down.shape
    rows, chips = groups * quarter, shards // cores
    head, tail = active[:LANES], active[LANES:]
    none = jnp.zeros_like(tail)
    upper, lower = jnp.concatenate([tail, none]), jnp.concatenate([none, tail])
    weights = down.reshape(chips, cores, rows, width)[:, pl.ds(side, 1)][:, 0]
    out[:, :rows] = nt_dot(weights.reshape(chips * rows, width), head).astype(out.dtype).reshape(chips, rows, LANES)
    packed = nt_dot(weights[:, : rows // 2].reshape(chips * rows // 2, width), upper) + nt_dot(
        weights[:, rows // 2 :].reshape(chips * rows // 2, width), lower
    )
    out[:, rows:] = packed.astype(out.dtype).reshape(chips, rows // 2, LANES)


def feed_forward(cores, where, normed, *refs):
    quarters, (up, down, active, away) = refs[:-4], refs[-4:]
    shards, groups, quarter, width = up.shape
    at, core, member = where[0], where[1], where[2]

    def place(weight, own, left, far_first, far_second, right):
        half = shards // 2
        for step, first, count, piece in (
            (0, 0, shards, own),
            (1, 0, shards, left),
            (2, 0, half, far_first),
            (2, half, half, far_second),
            (3, 0, shards, right),
        ):
            slot = lax.rem(at + step, groups)
            weight[pl.ds(first, count), pl.ds(slot, 1)] = piece[...][:, None]

    for value, mine, other in ((0, up, down), (1, down, up)):

        @pl.when(member == value)
        def _(mine=mine, other=other):
            place(mine, *quarters[:5])
            place(other, *quarters[5:])

    hidden = jnp.dot(
        normed[...], up[...].reshape(shards * groups * quarter, width), preferred_element_type=jnp.float32
    )
    rounded = jnp.square(jnp.maximum(hidden, 0.0)).astype(active.dtype)
    active[...] = rounded
    partial_sums(away, 1 - core, cores, rounded, down)


def own_side(cores, where, active, up, down, up_out, down_out, kept, sems):
    writes = [pltpu.make_async_copy(up, up_out, sems.at[0]), pltpu.make_async_copy(down, down_out, sems.at[1])]
    for write in writes:
        write.start()
    partial_sums(kept, where[1], cores, active[...], down)
    for write in writes:
        write.wait()


def added(a, b):
    return (a.astype(jnp.float32) + b.astype(jnp.float32)).astype(jnp.bfloat16)


def summed_up(arrived, out):
    rows, cols = out.shape
    total = arrived[0].astype(jnp.float32)
    for chip in range(1, arrived.shape[0]):
        total += arrived[chip].astype(jnp.float32)
    total = total.astype(out.dtype)
    out[:, :LANES] = total[:rows]
    tail = total[rows:]
    out[: rows // 2, LANES:] = tail[:, : cols - LANES]
    out[rows // 2 :, LANES:] = tail[:, cols - LANES :]


def local(tokens, norm_gain, up_trained, down_trained):
    chips, cores, groups = lax.axis_size("z"), lax.axis_size("core"), lax.axis_size("tp")
    shards = chips * cores
    rows_local, cols_local = up_trained.shape
    count, features = tokens.shape
    width = cols_local * groups // shards
    blocks = cols_local // (width * cores)
    quarter = rows_local // groups
    where = jnp.stack([lax.axis_index("tp"), lax.axis_index("core"), lax.axis_index("member")]).astype(jnp.int32)
    smem, vmem = pl.BlockSpec(memory_space=pltpu.SMEM), pl.BlockSpec(memory_space=pltpu.VMEM)
    first = lax.axis_index("member") == 0
    mine = jnp.where(first, norm_gain[:, None] * up_trained, down_trained).astype(jnp.bfloat16)
    pieces = mine.reshape(groups, quarter, blocks, cores, width).transpose(3, 0, 2, 1, 4)
    pieces = pieces.reshape(cores * groups, blocks, quarter, width)
    moved = lax.all_to_all(pieces, ("core", "tp"), 0, 0, tiled=True)
    moved = moved.reshape(cores, chips, quarter, width).transpose(1, 0, 2, 3)
    own = lax.all_to_all(moved, "z", 0, 0, tiled=True).reshape(shards, quarter, width)
    half = shards // 2
    values = tokens.astype(jnp.float32)
    scale = lax.rsqrt(jnp.mean(values * values, axis=1, keepdims=True) + epsilon)
    normed = (values * scale).astype(jnp.bfloat16)

    twin = lax.ppermute(own, "member", ring(PAIR, 1))
    right = lax.ppermute(own, "tp", ring(groups, 1))
    left = lax.ppermute(own, "tp", ring(groups, -1))
    twin_right = lax.ppermute(twin, "tp", ring(groups, 1))
    twin_left = lax.ppermute(twin, "tp", ring(groups, -1))
    far_first = lax.ppermute(right[:half], "tp", ring(groups, 1))
    far_second = lax.ppermute(left[half:], "tp", ring(groups, -1))
    twin_far_second = lax.ppermute(right[half:], ("member", "tp"), across(groups, 1))
    twin_far_first = lax.ppermute(left[:half], ("member", "tp"), across(groups, -1))
    served = jax.ShapeDtypeStruct((shards, groups, quarter, width), jnp.bfloat16)
    part = jax.ShapeDtypeStruct((chips, rows_local * count // LANES, LANES), jnp.bfloat16)
    up, down, active, away = pl.pallas_call(
        functools.partial(feed_forward, cores),
        out_shape=[served, served, jax.ShapeDtypeStruct((count, width), jnp.bfloat16), part],
        in_specs=[smem] + [vmem] * 11,
        out_specs=[vmem] * 4,
        compiler_params=pltpu.CompilerParams(vmem_limit_bytes=24 << 20),
        cost_estimate=pl.CostEstimate(
            flops=3 * count * features * width, bytes_accessed=8 * features * width, transcendentals=0
        ),
        name="feed_forward",
    )(
        where, normed, own, left, far_first, far_second, right,
        twin, twin_left, twin_far_first, twin_far_second, twin_right,
    )
    up_serving, down_serving, kept = pl.pallas_call(
        functools.partial(own_side, cores),
        out_shape=[served, served, part],
        in_specs=[smem] + [vmem] * 3,
        out_specs=[pl.BlockSpec(memory_space=pl.ANY)] * 2 + [vmem],
        scratch_shapes=[pltpu.SemaphoreType.DMA((2,))],
        compiler_params=pltpu.CompilerParams(vmem_limit_bytes=16 << 20),
        cost_estimate=pl.CostEstimate(
            flops=count * features * width, bytes_accessed=8 * features * width, transcendentals=0
        ),
        name="own_side",
    )(where, active, up, down)
    swapped = lax.ppermute(away, "core", ring(cores, 1))
    arrived = lax.all_to_all(added(kept, swapped), "z", 0, 0, tiled=True)
    out = pl.pallas_call(
        summed_up,
        out_shape=jax.ShapeDtypeStruct((rows_local, count), jnp.bfloat16),
        in_specs=[vmem],
        out_specs=vmem,
        compiler_params=pltpu.CompilerParams(vmem_limit_bytes=8 << 20),
        name="summed_up",
    )(arrived).T
    return (up_serving.reshape(features, width), down_serving.reshape(features, width), out)


def solution(mesh):
    sizes = mesh.shape
    devices = mesh.devices.reshape(sizes["grp"] // PAIR, PAIR, sizes["fs"] // CORES, CORES, sizes["tp"])
    split = jax.sharding.Mesh(devices, ("pair", "member", "z", "core", "tp"))
    grp, fs = ("pair", "member"), ("z", "core")
    in_specs = (P((*grp, "tp"), None), P(fs), P(fs, "tp"), P(fs, "tp"))
    out_specs = (P(grp, fs), P(grp, fs), P((*grp, "tp"), fs))

    return jax.shard_map(local, mesh=split, in_specs=in_specs, out_specs=out_specs, check_vma=False)
```

```python
import functools

import jax
import jax.numpy as jnp
from jax import lax
from jax.experimental import pallas as pl
from jax.experimental.pallas import tpu as pltpu
from jax.sharding import PartitionSpec as P


epsilon = 1e-06
CORES = 2
PAIR = 2
LANES = 128


def ring(devices, step):
    return [(i, (i + step) % devices) for i in range(devices)]


def across(devices, step):
    return [
        (member * devices + i, (1 - member) * devices + (i + step) % devices)
        for member in range(PAIR)
        for i in range(devices)
    ]


def nt_dot(a, b):
    return lax.dot_general(a, b, (((1,), (1,)), ((), ())), preferred_element_type=jnp.float32)


def partial_sums(out, side, cores, active, down):
    shards, groups, quarter, width = down.shape
    rows, chips = groups * quarter, shards // cores
    head, tail = active[:LANES], active[LANES:]
    none = jnp.zeros_like(tail)
    upper, lower = jnp.concatenate([tail, none]), jnp.concatenate([none, tail])
    weights = down.reshape(chips, cores, rows, width)[:, pl.ds(side, 1)][:, 0]
    out[:, :rows] = nt_dot(weights.reshape(chips * rows, width), head).astype(out.dtype).reshape(chips, rows, LANES)
    packed = nt_dot(weights[:, : rows // 2].reshape(chips * rows // 2, width), upper) + nt_dot(
        weights[:, rows // 2 :].reshape(chips * rows // 2, width), lower
    )
    out[:, rows:] = packed.astype(out.dtype).reshape(chips, rows // 2, LANES)


def feed_forward(cores, where, normed, *refs):
    quarters, (up, down, active, away) = refs[:-4], refs[-4:]
    shards, groups, quarter, width = up.shape
    at, core, member = where[0], where[1], where[2]

    def place(weight, *pieces):
        for step, parts in enumerate(pieces):
            slot, first = lax.rem(at + step, groups), 0
            for part in parts:
                count = part.shape[0]
                weight[pl.ds(first, count), pl.ds(slot, 1)] = part[...][:, None]
                first += count

    own, left, far, right, twin, *rest, twin_right = quarters
    for value, mine, other in ((0, up, down), (1, down, up)):

        @pl.when(member == value)
        def _(mine=mine, other=other):
            place(mine, [own], [left], [far], [right])
            place(other, [twin], rest[:2], rest[2:], [twin_right])

    hidden = jnp.dot(
        normed[...], up[...].reshape(shards * groups * quarter, width), preferred_element_type=jnp.float32
    )
    rounded = jnp.square(jnp.maximum(hidden, 0.0)).astype(active.dtype)
    active[...] = rounded
    partial_sums(away, 1 - core, cores, rounded, down)


def own_side(cores, where, active, up, down, up_out, down_out, kept, sems):
    writes = [pltpu.make_async_copy(up, up_out, sems.at[0]), pltpu.make_async_copy(down, down_out, sems.at[1])]
    for write in writes:
        write.start()
    partial_sums(kept, where[1], cores, active[...], down)
    for write in writes:
        write.wait()


def added(a, b):
    return (a.astype(jnp.float32) + b.astype(jnp.float32)).astype(jnp.bfloat16)


def summed_up(arrived, out):
    rows, cols = out.shape
    total = arrived[0].astype(jnp.float32)
    for chip in range(1, arrived.shape[0]):
        total += arrived[chip].astype(jnp.float32)
    total = total.astype(out.dtype)
    out[:, :LANES] = total[:rows]
    tail = total[rows:]
    out[: rows // 2, LANES:] = tail[:, : cols - LANES]
    out[rows // 2 :, LANES:] = tail[:, cols - LANES :]


def local(tokens, norm_gain, up_trained, down_trained):
    chips, cores, groups = lax.axis_size("z"), lax.axis_size("core"), lax.axis_size("tp")
    shards = chips * cores
    rows_local, cols_local = up_trained.shape
    count, features = tokens.shape
    width = cols_local * groups // shards
    blocks = cols_local // (width * cores)
    quarter = rows_local // groups
    where = jnp.stack([lax.axis_index("tp"), lax.axis_index("core"), lax.axis_index("member")]).astype(jnp.int32)
    smem, vmem = pl.BlockSpec(memory_space=pltpu.SMEM), pl.BlockSpec(memory_space=pltpu.VMEM)
    first = lax.axis_index("member") == 0
    mine = jnp.where(first, norm_gain[:, None] * up_trained, down_trained).astype(jnp.bfloat16)
    pieces = mine.reshape(groups, quarter, blocks, cores, width).transpose(3, 0, 2, 1, 4)
    pieces = pieces.reshape(cores * groups, blocks, quarter, width)
    moved = lax.all_to_all(pieces, ("core", "tp"), 0, 0, tiled=True)
    moved = moved.reshape(cores, chips, quarter, width).transpose(1, 0, 2, 3)
    own = lax.all_to_all(moved, "z", 0, 0, tiled=True).reshape(shards, quarter, width)
    values = tokens.astype(jnp.float32)
    scale = lax.rsqrt(jnp.mean(values * values, axis=1, keepdims=True) + epsilon)
    normed = (values * scale).astype(jnp.bfloat16)

    twin = lax.ppermute(own, "member", ring(PAIR, 1))
    left = lax.ppermute(own, "tp", ring(groups, -1))
    right = lax.ppermute(own, "tp", ring(groups, 1))
    cut, far_cut = shards * 5 // 8, shards * 3 // 8
    twin_right = lax.ppermute(twin, "tp", ring(groups, 1))
    far = lax.ppermute(left, "tp", ring(groups, -1))
    twin_left_first = lax.ppermute(left[:cut], "member", ring(PAIR, 1))
    twin_far_second = lax.ppermute(right[far_cut:], ("member", "tp"), across(groups, 1))
    twin_left_second = lax.ppermute(twin[cut:], "tp", ring(groups, -1))
    twin_far_first = lax.ppermute(left[:far_cut], ("member", "tp"), across(groups, -1))
    served = jax.ShapeDtypeStruct((shards, groups, quarter, width), jnp.bfloat16)
    part = jax.ShapeDtypeStruct((chips, rows_local * count // LANES, LANES), jnp.bfloat16)
    up, down, active, away = pl.pallas_call(
        functools.partial(feed_forward, cores),
        out_shape=[served, served, jax.ShapeDtypeStruct((count, width), jnp.bfloat16), part],
        in_specs=[smem] + [vmem] * 11,
        out_specs=[vmem] * 4,
        compiler_params=pltpu.CompilerParams(vmem_limit_bytes=24 << 20),
        cost_estimate=pl.CostEstimate(
            flops=3 * count * features * width, bytes_accessed=8 * features * width, transcendentals=0
        ),
        name="feed_forward",
    )(
        where, normed, own, left, far, right,
        twin, twin_left_first, twin_left_second, twin_far_first, twin_far_second, twin_right,
    )
    up_serving, down_serving, kept = pl.pallas_call(
        functools.partial(own_side, cores),
        out_shape=[served, served, part],
        in_specs=[smem] + [vmem] * 3,
        out_specs=[pl.BlockSpec(memory_space=pl.ANY)] * 2 + [vmem],
        scratch_shapes=[pltpu.SemaphoreType.DMA((2,))],
        compiler_params=pltpu.CompilerParams(vmem_limit_bytes=16 << 20),
        cost_estimate=pl.CostEstimate(
            flops=count * features * width, bytes_accessed=8 * features * width, transcendentals=0
        ),
        name="own_side",
    )(where, active, up, down)
    swapped = lax.ppermute(away, "core", ring(cores, 1))
    arrived = lax.all_to_all(added(kept, swapped), "z", 0, 0, tiled=True)
    out = pl.pallas_call(
        summed_up,
        out_shape=jax.ShapeDtypeStruct((rows_local, count), jnp.bfloat16),
        in_specs=[vmem],
        out_specs=vmem,
        compiler_params=pltpu.CompilerParams(vmem_limit_bytes=8 << 20),
        name="summed_up",
    )(arrived).T
    return (up_serving.reshape(features, width), down_serving.reshape(features, width), out)


def solution(mesh):
    sizes = mesh.shape
    devices = mesh.devices.reshape(sizes["grp"] // PAIR, PAIR, sizes["fs"] // CORES, CORES, sizes["tp"])
    split = jax.sharding.Mesh(devices, ("pair", "member", "z", "core", "tp"))
    grp, fs = ("pair", "member"), ("z", "core")
    in_specs = (P((*grp, "tp"), None), P(fs), P(fs, "tp"), P(fs, "tp"))
    out_specs = (P(grp, fs), P(grp, fs), P((*grp, "tp"), fs))

    return jax.shard_map(local, mesh=split, in_specs=in_specs, out_specs=out_specs, check_vma=False)
```

```python
import functools

import jax
import jax.numpy as jnp
from jax import lax
from jax.experimental import pallas as pl
from jax.experimental.pallas import tpu as pltpu
from jax.sharding import PartitionSpec as P


epsilon = 1e-06
CORES = 2
PAIR = 2
LANES = 128


def ring(devices, step):
    return [(i, (i + step) % devices) for i in range(devices)]


def across(devices, step):
    return [
        (member * devices + i, (1 - member) * devices + (i + step) % devices)
        for member in range(PAIR)
        for i in range(devices)
    ]


def nt_dot(a, b):
    return lax.dot_general(a, b, (((1,), (1,)), ((), ())), preferred_element_type=jnp.float32)


def from_both_ends(chips):
    return [i // 2 if i % 2 == 0 else chips - 1 - i // 2 for i in range(chips)]


def partial_sums(out, side, cores, active, down):
    shards, groups, quarter, width = down.shape
    rows, chips = groups * quarter, shards // cores
    head, tail = active[:LANES], active[LANES:]
    none = jnp.zeros_like(tail)
    upper, lower = jnp.concatenate([tail, none]), jnp.concatenate([none, tail])
    weights = down.reshape(chips, cores, rows, width)[:, pl.ds(side, 1)][:, 0]
    wide = nt_dot(weights.reshape(chips * rows, width), head).astype(out.dtype).reshape(chips, rows, LANES)
    packed = nt_dot(weights[:, : rows // 2].reshape(chips * rows // 2, width), upper) + nt_dot(
        weights[:, rows // 2 :].reshape(chips * rows // 2, width), lower
    )
    packed = packed.astype(out.dtype).reshape(chips, rows // 2, LANES)
    for place, chip in enumerate(from_both_ends(chips)):
        out[place, :rows] = wide[chip]
        out[place, rows:] = packed[chip]


def feed_forward(cores, where, normed, *refs):
    quarters, (up, down, active, away) = refs[:-4], refs[-4:]
    shards, groups, quarter, width = up.shape
    at, core, member = where[0], where[1], where[2]

    def place(weight, *pieces):
        for step, parts in enumerate(pieces):
            slot, first = lax.rem(at + step, groups), 0
            for part in parts:
                count = part.shape[0]
                weight[pl.ds(first, count), pl.ds(slot, 1)] = part[...][:, None]
                first += count

    own, left, far, right, twin, *rest, twin_right = quarters
    for value, mine, other in ((0, up, down), (1, down, up)):

        @pl.when(member == value)
        def _(mine=mine, other=other):
            place(mine, [own], [left], [far], [right])
            place(other, [twin], rest[:2], rest[2:], [twin_right])

    hidden = jnp.dot(
        normed[...], up[...].reshape(shards * groups * quarter, width), preferred_element_type=jnp.float32
    )
    rounded = jnp.square(jnp.maximum(hidden, 0.0)).astype(active.dtype)
    active[...] = rounded
    partial_sums(away, 1 - core, cores, rounded, down)


def own_side(cores, where, active, up, down, up_out, down_out, kept, sems):
    writes = [pltpu.make_async_copy(up, up_out, sems.at[0]), pltpu.make_async_copy(down, down_out, sems.at[1])]
    for write in writes:
        write.start()
    partial_sums(kept, where[1], cores, active[...], down)
    for write in writes:
        write.wait()


def added(a, b):
    return (a.astype(jnp.float32) + b.astype(jnp.float32)).astype(jnp.bfloat16)


def summed_up(arrived, out):
    rows, cols = out.shape
    total = arrived[0].astype(jnp.float32)
    for chip in range(1, arrived.shape[0]):
        total += arrived[chip].astype(jnp.float32)
    total = total.astype(out.dtype)
    out[:, :LANES] = total[:rows]
    tail = total[rows:]
    out[: rows // 2, LANES:] = tail[:, : cols - LANES]
    out[rows // 2 :, LANES:] = tail[:, cols - LANES :]


def local(tokens, norm_gain, up_trained, down_trained):
    chips, cores, groups = lax.axis_size("z"), lax.axis_size("core"), lax.axis_size("tp")
    shards = chips * cores
    rows_local, cols_local = up_trained.shape
    count, features = tokens.shape
    width = cols_local * groups // shards
    blocks = cols_local // (width * cores)
    quarter = rows_local // groups
    where = jnp.stack([lax.axis_index("tp"), lax.axis_index("core"), lax.axis_index("member")]).astype(jnp.int32)
    smem, vmem = pl.BlockSpec(memory_space=pltpu.SMEM), pl.BlockSpec(memory_space=pltpu.VMEM)
    first = lax.axis_index("member") == 0
    mine = jnp.where(first, norm_gain[:, None] * up_trained, down_trained).astype(jnp.bfloat16)
    pieces = mine.reshape(groups, quarter, blocks, cores, width).transpose(3, 0, 2, 1, 4)
    pieces = pieces.reshape(cores * groups, blocks, quarter, width)
    moved = lax.all_to_all(pieces, ("core", "tp"), 0, 0, tiled=True)
    moved = moved.reshape(cores, chips, quarter, width).transpose(1, 0, 2, 3)
    own = lax.all_to_all(moved, "z", 0, 0, tiled=True).reshape(shards, quarter, width)
    values = tokens.astype(jnp.float32)
    scale = lax.rsqrt(jnp.mean(values * values, axis=1, keepdims=True) + epsilon)
    normed = (values * scale).astype(jnp.bfloat16)

    twin = lax.ppermute(own, "member", ring(PAIR, 1))
    left = lax.ppermute(own, "tp", ring(groups, -1))
    right = lax.ppermute(own, "tp", ring(groups, 1))
    cut, far_cut = shards * 5 // 8, shards * 3 // 8
    twin_right = lax.ppermute(twin, "tp", ring(groups, 1))
    far = lax.ppermute(left, "tp", ring(groups, -1))
    twin_left_first = lax.ppermute(left[:cut], "member", ring(PAIR, 1))
    twin_far_second = lax.ppermute(right[far_cut:], ("member", "tp"), across(groups, 1))
    twin_left_second = lax.ppermute(twin[cut:], "tp", ring(groups, -1))
    twin_far_first = lax.ppermute(left[:far_cut], ("member", "tp"), across(groups, -1))
    served = jax.ShapeDtypeStruct((shards, groups, quarter, width), jnp.bfloat16)
    part = jax.ShapeDtypeStruct((chips, rows_local * count // LANES, LANES), jnp.bfloat16)
    up, down, active, away = pl.pallas_call(
        functools.partial(feed_forward, cores),
        out_shape=[served, served, jax.ShapeDtypeStruct((count, width), jnp.bfloat16), part],
        in_specs=[smem] + [vmem] * 11,
        out_specs=[vmem] * 4,
        compiler_params=pltpu.CompilerParams(vmem_limit_bytes=24 << 20),
        cost_estimate=pl.CostEstimate(
            flops=3 * count * features * width, bytes_accessed=8 * features * width, transcendentals=0
        ),
        name="feed_forward",
    )(
        where, normed, own, left, far, right,
        twin, twin_left_first, twin_left_second, twin_far_first, twin_far_second, twin_right,
    )
    up_serving, down_serving, kept = pl.pallas_call(
        functools.partial(own_side, cores),
        out_shape=[served, served, part],
        in_specs=[smem] + [vmem] * 3,
        out_specs=[pl.BlockSpec(memory_space=pl.ANY)] * 2 + [vmem],
        scratch_shapes=[pltpu.SemaphoreType.DMA((2,))],
        compiler_params=pltpu.CompilerParams(vmem_limit_bytes=16 << 20),
        cost_estimate=pl.CostEstimate(
            flops=count * features * width, bytes_accessed=8 * features * width, transcendentals=0
        ),
        name="own_side",
    )(where, active, up, down)
    swapped = lax.ppermute(away, "core", ring(cores, 1))
    order = [from_both_ends(chips)]
    arrived = lax.all_to_all(added(kept, swapped), "z", 0, 0, axis_index_groups=order, tiled=True)
    out = pl.pallas_call(
        summed_up,
        out_shape=jax.ShapeDtypeStruct((rows_local, count), jnp.bfloat16),
        in_specs=[vmem],
        out_specs=vmem,
        compiler_params=pltpu.CompilerParams(vmem_limit_bytes=8 << 20),
        name="summed_up",
    )(arrived).T
    return (up_serving.reshape(features, width), down_serving.reshape(features, width), out)


def solution(mesh):
    sizes = mesh.shape
    devices = mesh.devices.reshape(sizes["grp"] // PAIR, PAIR, sizes["fs"] // CORES, CORES, sizes["tp"])
    split = jax.sharding.Mesh(devices, ("pair", "member", "z", "core", "tp"))
    grp, fs = ("pair", "member"), ("z", "core")
    in_specs = (P((*grp, "tp"), None), P(fs), P(fs, "tp"), P(fs, "tp"))
    out_specs = (P(grp, fs), P(grp, fs), P((*grp, "tp"), fs))

    return jax.shard_map(local, mesh=split, in_specs=in_specs, out_specs=out_specs, check_vma=False)
```

```python
import functools

import jax
import jax.numpy as jnp
from jax import lax
from jax.experimental import pallas as pl
from jax.experimental.pallas import tpu as pltpu
from jax.sharding import PartitionSpec as P


epsilon = 1e-06
CORES = 2
PAIR = 2
LANES = 128


def ring(devices, step):
    return [(i, (i + step) % devices) for i in range(devices)]


def across(devices, step):
    return [
        (member * devices + i, (1 - member) * devices + (i + step) % devices)
        for member in range(PAIR)
        for i in range(devices)
    ]


def nt_dot(a, b):
    return lax.dot_general(a, b, (((1,), (1,)), ((), ())), preferred_element_type=jnp.float32)


def partial_sums(out, parity, side, cores, active, down):
    shards, groups, quarter, width = down.shape
    rows, blocks = groups * quarter, shards // cores // 2
    head, tail = active[:LANES], active[LANES:]
    none = jnp.zeros_like(tail)
    upper, lower = jnp.concatenate([tail, none]), jnp.concatenate([none, tail])
    for part in (1, 0):
        on = lax.rem(parity + part, 2) * cores + side
        weights = down.reshape(blocks, 2 * cores, rows, width)[:, pl.ds(on, 1)][:, 0]
        wide = nt_dot(weights.reshape(blocks * rows, width), head).astype(out.dtype).reshape(blocks, rows, LANES)
        packed = nt_dot(weights[:, : rows // 2].reshape(blocks * rows // 2, width), upper) + nt_dot(
            weights[:, rows // 2 :].reshape(blocks * rows // 2, width), lower
        )
        packed = packed.astype(out.dtype).reshape(blocks, rows // 2, LANES)
        for block in range(blocks):
            out[part, blocks - 1 - block, :rows] = wide[block]
            out[part, blocks - 1 - block, rows:] = packed[block]


def feed_forward(cores, where, normed, *refs):
    quarters, (up, down, active, away) = refs[:-4], refs[-4:]
    shards, groups, quarter, width = up.shape
    at, core, member, parity = where[0], where[1], where[2], where[3]

    def place(weight, *pieces):
        for step, parts in enumerate(pieces):
            slot, first = lax.rem(at + step, groups), 0
            for part in parts:
                count = part.shape[0]
                weight[pl.ds(first, count), pl.ds(slot, 1)] = part[...][:, None]
                first += count

    own, left, far, right, twin, *rest, twin_right = quarters
    for value, mine, other in ((0, up, down), (1, down, up)):

        @pl.when(member == value)
        def _(mine=mine, other=other):
            place(mine, [own], [left], [far], [right])
            place(other, [twin], rest[:2], rest[2:], [twin_right])

    hidden = jnp.dot(
        normed[...], up[...].reshape(shards * groups * quarter, width), preferred_element_type=jnp.float32
    )
    rounded = jnp.square(jnp.maximum(hidden, 0.0)).astype(active.dtype)
    active[...] = rounded
    partial_sums(away, parity, 1 - core, cores, rounded, down)


def own_side(cores, where, active, up, down, up_out, down_out, kept, sems):
    writes = [pltpu.make_async_copy(up, up_out, sems.at[0]), pltpu.make_async_copy(down, down_out, sems.at[1])]
    for write in writes:
        write.start()
    partial_sums(kept, where[3], where[1], cores, active[...], down)
    for write in writes:
        write.wait()


def added(a, b):
    return (a.astype(jnp.float32) + b.astype(jnp.float32)).astype(jnp.bfloat16)


def summed_up(arrived, out):
    rows, cols = out.shape
    total = arrived[0].astype(jnp.float32)
    for chip in range(1, arrived.shape[0]):
        total += arrived[chip].astype(jnp.float32)
    total = total.astype(out.dtype)
    out[:, :LANES] = total[:rows]
    tail = total[rows:]
    out[: rows // 2, LANES:] = tail[:, : cols - LANES]
    out[rows // 2 :, LANES:] = tail[:, cols - LANES :]


def local(tokens, norm_gain, up_trained, down_trained):
    chips, cores, groups = lax.axis_size("z"), lax.axis_size("core"), lax.axis_size("tp")
    shards = chips * cores
    rows_local, cols_local = up_trained.shape
    count, features = tokens.shape
    width = cols_local * groups // shards
    blocks = cols_local // (width * cores)
    quarter = rows_local // groups
    where = jnp.stack([lax.axis_index("tp"), lax.axis_index("core"), lax.axis_index("member"), lax.axis_index("z") % 2]).astype(jnp.int32)
    smem, vmem = pl.BlockSpec(memory_space=pltpu.SMEM), pl.BlockSpec(memory_space=pltpu.VMEM)
    first = lax.axis_index("member") == 0
    mine = jnp.where(first, norm_gain[:, None] * up_trained, down_trained).astype(jnp.bfloat16)
    pieces = mine.reshape(groups, quarter, blocks, cores, width).transpose(3, 0, 2, 1, 4)
    pieces = pieces.reshape(cores * groups, blocks, quarter, width)
    moved = lax.all_to_all(pieces, ("core", "tp"), 0, 0, tiled=True)
    moved = moved.reshape(cores, chips, quarter, width).transpose(1, 0, 2, 3)
    own = lax.all_to_all(moved, "z", 0, 0, tiled=True).reshape(shards, quarter, width)
    values = tokens.astype(jnp.float32)
    scale = lax.rsqrt(jnp.mean(values * values, axis=1, keepdims=True) + epsilon)
    normed = (values * scale).astype(jnp.bfloat16)

    twin = lax.ppermute(own, "member", ring(PAIR, 1))
    left = lax.ppermute(own, "tp", ring(groups, -1))
    right = lax.ppermute(own, "tp", ring(groups, 1))
    cut, far_cut = shards * 5 // 8, shards * 3 // 8
    twin_right = lax.ppermute(twin, "tp", ring(groups, 1))
    far = lax.ppermute(left, "tp", ring(groups, -1))
    twin_left_first = lax.ppermute(left[:cut], "member", ring(PAIR, 1))
    twin_far_second = lax.ppermute(right[far_cut:], ("member", "tp"), across(groups, 1))
    twin_left_second = lax.ppermute(twin[cut:], "tp", ring(groups, -1))
    twin_far_first = lax.ppermute(left[:far_cut], ("member", "tp"), across(groups, -1))
    served = jax.ShapeDtypeStruct((shards, groups, quarter, width), jnp.bfloat16)
    part = jax.ShapeDtypeStruct((2, chips // 2, rows_local * count // LANES, LANES), jnp.bfloat16)
    up, down, active, away = pl.pallas_call(
        functools.partial(feed_forward, cores),
        out_shape=[served, served, jax.ShapeDtypeStruct((count, width), jnp.bfloat16), part],
        in_specs=[smem] + [vmem] * 11,
        out_specs=[vmem] * 4,
        compiler_params=pltpu.CompilerParams(vmem_limit_bytes=24 << 20),
        cost_estimate=pl.CostEstimate(
            flops=3 * count * features * width, bytes_accessed=8 * features * width, transcendentals=0
        ),
        name="feed_forward",
    )(
        where, normed, own, left, far, right,
        twin, twin_left_first, twin_left_second, twin_far_first, twin_far_second, twin_right,
    )
    up_serving, down_serving, kept = pl.pallas_call(
        functools.partial(own_side, cores),
        out_shape=[served, served, part],
        in_specs=[smem] + [vmem] * 3,
        out_specs=[pl.BlockSpec(memory_space=pl.ANY)] * 2 + [vmem],
        scratch_shapes=[pltpu.SemaphoreType.DMA((2,))],
        compiler_params=pltpu.CompilerParams(vmem_limit_bytes=16 << 20),
        cost_estimate=pl.CostEstimate(
            flops=count * features * width, bytes_accessed=8 * features * width, transcendentals=0
        ),
        name="own_side",
    )(where, active, up, down)
    swapped = lax.ppermute(away, "core", ring(cores, 1))
    leaving = added(kept[1], swapped[1])
    mid = chips // 4
    up_one = lax.ppermute(leaving[:mid], "z", ring(chips, 1))
    down_one = lax.ppermute(leaving[mid:], "z", ring(chips, -1))
    summed = added(added(kept[0], swapped[0]), jnp.concatenate([up_one, down_one]))
    same_parity = [list(range(chips - 2 + first, -1, -2)) for first in range(2)]
    arrived = lax.all_to_all(summed, "z", 0, 0, axis_index_groups=same_parity, tiled=True)
    out = pl.pallas_call(
        summed_up,
        out_shape=jax.ShapeDtypeStruct((rows_local, count), jnp.bfloat16),
        in_specs=[vmem],
        out_specs=vmem,
        compiler_params=pltpu.CompilerParams(vmem_limit_bytes=8 << 20),
        name="summed_up",
    )(arrived).T
    return (up_serving.reshape(features, width), down_serving.reshape(features, width), out)


def solution(mesh):
    sizes = mesh.shape
    devices = mesh.devices.reshape(sizes["grp"] // PAIR, PAIR, sizes["fs"] // CORES, CORES, sizes["tp"])
    split = jax.sharding.Mesh(devices, ("pair", "member", "z", "core", "tp"))
    grp, fs = ("pair", "member"), ("z", "core")
    in_specs = (P((*grp, "tp"), None), P(fs), P(fs, "tp"), P(fs, "tp"))
    out_specs = (P(grp, fs), P(grp, fs), P((*grp, "tp"), fs))

    return jax.shard_map(local, mesh=split, in_specs=in_specs, out_specs=out_specs, check_vma=False)
```

```python
import functools

import jax
import jax.numpy as jnp
from jax import lax
from jax.experimental import pallas as pl
from jax.experimental.pallas import tpu as pltpu
from jax.sharding import PartitionSpec as P


epsilon = 1e-06
CORES = 2
PAIR = 2
LANES = 128


def ring(devices, step):
    return [(i, (i + step) % devices) for i in range(devices)]


def across(devices, step):
    return [
        (member * devices + i, (1 - member) * devices + (i + step) % devices)
        for member in range(PAIR)
        for i in range(devices)
    ]


def nt_dot(a, b):
    return lax.dot_general(a, b, (((1,), (1,)), ((), ())), preferred_element_type=jnp.float32)


def places(blocks, odd):
    return [(blocks - 1 - (3 if odd else 1) * block) % blocks for block in range(blocks)]


def partial_sums(out, parity, side, cores, active, down):
    shards, groups, quarter, width = down.shape
    rows, blocks = groups * quarter, shards // cores // 2
    head, tail = active[:LANES], active[LANES:]
    none = jnp.zeros_like(tail)
    upper, lower = jnp.concatenate([tail, none]), jnp.concatenate([none, tail])
    for part in (1, 0):
        on = lax.rem(parity + part, 2) * cores + side
        weights = down.reshape(blocks, 2 * cores, rows, width)[:, pl.ds(on, 1)][:, 0]
        wide = nt_dot(weights.reshape(blocks * rows, width), head).astype(out.dtype).reshape(blocks, rows, LANES)
        packed = nt_dot(weights[:, : rows // 2].reshape(blocks * rows // 2, width), upper) + nt_dot(
            weights[:, rows // 2 :].reshape(blocks * rows // 2, width), lower
        )
        packed = packed.astype(out.dtype).reshape(blocks, rows // 2, LANES)
        odd = lax.rem(parity + part, 2)
        for block, (even_place, odd_place) in enumerate(zip(places(blocks, False), places(blocks, True))):
            place = pl.ds(jnp.where(odd == 0, even_place, odd_place), 1)
            out[part, place, :rows] = wide[block][None]
            out[part, place, rows:] = packed[block][None]


def feed_forward(cores, where, normed, *refs):
    quarters, (up, down, active, away) = refs[:-4], refs[-4:]
    shards, groups, quarter, width = up.shape
    at, core, member, parity = where[0], where[1], where[2], where[3]

    def place(weight, *pieces):
        for step, parts in enumerate(pieces):
            slot, first = lax.rem(at + step, groups), 0
            for part in parts:
                count = part.shape[0]
                weight[pl.ds(first, count), pl.ds(slot, 1)] = part[...][:, None]
                first += count

    own, left, far, right, twin, *rest, twin_right = quarters
    for value, mine, other in ((0, up, down), (1, down, up)):

        @pl.when(member == value)
        def _(mine=mine, other=other):
            place(mine, [own], [left], [far], [right])
            place(other, [twin], rest[:2], rest[2:], [twin_right])

    hidden = jnp.dot(
        normed[...], up[...].reshape(shards * groups * quarter, width), preferred_element_type=jnp.float32
    )
    rounded = jnp.square(jnp.maximum(hidden, 0.0)).astype(active.dtype)
    active[...] = rounded
    partial_sums(away, parity, 1 - core, cores, rounded, down)


def own_side(cores, where, active, up, down, up_out, down_out, kept, sems):
    writes = [pltpu.make_async_copy(up, up_out, sems.at[0]), pltpu.make_async_copy(down, down_out, sems.at[1])]
    for write in writes:
        write.start()
    partial_sums(kept, where[3], where[1], cores, active[...], down)
    for write in writes:
        write.wait()


def added(a, b):
    return (a.astype(jnp.float32) + b.astype(jnp.float32)).astype(jnp.bfloat16)


def summed_up(arrived, out):
    rows, cols = out.shape
    total = arrived[0].astype(jnp.float32)
    for chip in range(1, arrived.shape[0]):
        total += arrived[chip].astype(jnp.float32)
    total = total.astype(out.dtype)
    out[:, :LANES] = total[:rows]
    tail = total[rows:]
    out[: rows // 2, LANES:] = tail[:, : cols - LANES]
    out[rows // 2 :, LANES:] = tail[:, cols - LANES :]


def local(tokens, norm_gain, up_trained, down_trained):
    chips, cores, groups = lax.axis_size("z"), lax.axis_size("core"), lax.axis_size("tp")
    shards = chips * cores
    rows_local, cols_local = up_trained.shape
    count, features = tokens.shape
    width = cols_local * groups // shards
    blocks = cols_local // (width * cores)
    quarter = rows_local // groups
    where = jnp.stack([lax.axis_index("tp"), lax.axis_index("core"), lax.axis_index("member"), lax.axis_index("z") % 2]).astype(jnp.int32)
    smem, vmem = pl.BlockSpec(memory_space=pltpu.SMEM), pl.BlockSpec(memory_space=pltpu.VMEM)
    first = lax.axis_index("member") == 0
    mine = jnp.where(first, norm_gain[:, None] * up_trained, down_trained).astype(jnp.bfloat16)
    pieces = mine.reshape(groups, quarter, blocks, cores, width).transpose(3, 0, 2, 1, 4)
    pieces = pieces.reshape(cores * groups, blocks, quarter, width)
    moved = lax.all_to_all(pieces, ("core", "tp"), 0, 0, tiled=True)
    moved = moved.reshape(cores, chips, quarter, width).transpose(1, 0, 2, 3)
    own = lax.all_to_all(moved, "z", 0, 0, tiled=True).reshape(shards, quarter, width)
    values = tokens.astype(jnp.float32)
    scale = lax.rsqrt(jnp.mean(values * values, axis=1, keepdims=True) + epsilon)
    normed = (values * scale).astype(jnp.bfloat16)

    twin = lax.ppermute(own, "member", ring(PAIR, 1))
    left = lax.ppermute(own, "tp", ring(groups, -1))
    right = lax.ppermute(own, "tp", ring(groups, 1))
    cut, far_cut = shards // 2, shards // 4
    twin_right = lax.ppermute(twin, "tp", ring(groups, 1))
    far = lax.ppermute(left, "tp", ring(groups, -1))
    twin_left_first = lax.ppermute(left[:cut], "member", ring(PAIR, 1))
    twin_far_second = lax.ppermute(right[far_cut:], ("member", "tp"), across(groups, 1))
    twin_left_second = lax.ppermute(twin[cut:], "tp", ring(groups, -1))
    twin_far_first = lax.ppermute(left[:far_cut], ("member", "tp"), across(groups, -1))
    served = jax.ShapeDtypeStruct((shards, groups, quarter, width), jnp.bfloat16)
    part = jax.ShapeDtypeStruct((2, chips // 2, rows_local * count // LANES, LANES), jnp.bfloat16)
    up, down, active, away = pl.pallas_call(
        functools.partial(feed_forward, cores),
        out_shape=[served, served, jax.ShapeDtypeStruct((count, width), jnp.bfloat16), part],
        in_specs=[smem] + [vmem] * 11,
        out_specs=[vmem] * 4,
        compiler_params=pltpu.CompilerParams(vmem_limit_bytes=24 << 20),
        cost_estimate=pl.CostEstimate(
            flops=3 * count * features * width, bytes_accessed=8 * features * width, transcendentals=0
        ),
        name="feed_forward",
    )(
        where, normed, own, left, far, right,
        twin, twin_left_first, twin_left_second, twin_far_first, twin_far_second, twin_right,
    )
    up_serving, down_serving, kept = pl.pallas_call(
        functools.partial(own_side, cores),
        out_shape=[served, served, part],
        in_specs=[smem] + [vmem] * 3,
        out_specs=[pl.BlockSpec(memory_space=pl.ANY)] * 2 + [vmem],
        scratch_shapes=[pltpu.SemaphoreType.DMA((2,))],
        compiler_params=pltpu.CompilerParams(vmem_limit_bytes=16 << 20),
        cost_estimate=pl.CostEstimate(
            flops=count * features * width, bytes_accessed=8 * features * width, transcendentals=0
        ),
        name="own_side",
    )(where, active, up, down)
    swapped = lax.ppermute(away, "core", ring(cores, 1))
    leaving = added(kept[1], swapped[1])
    mid = chips // 4
    up_one = lax.ppermute(leaving[:mid], "z", ring(chips, 1))
    down_one = lax.ppermute(leaving[mid:], "z", ring(chips, -1))
    summed = added(added(kept[0], swapped[0]), jnp.concatenate([up_one, down_one]))
    same_parity = [
        sorted(range(odd, chips, 2), key=lambda chip: places(chips // 2, odd)[chip // 2]) for odd in range(2)
    ]
    arrived = lax.all_to_all(summed, "z", 0, 0, axis_index_groups=same_parity, tiled=True)
    out = pl.pallas_call(
        summed_up,
        out_shape=jax.ShapeDtypeStruct((rows_local, count), jnp.bfloat16),
        in_specs=[vmem],
        out_specs=vmem,
        compiler_params=pltpu.CompilerParams(vmem_limit_bytes=8 << 20),
        name="summed_up",
    )(arrived).T
    return (up_serving.reshape(features, width), down_serving.reshape(features, width), out)


def solution(mesh):
    sizes = mesh.shape
    devices = mesh.devices.reshape(sizes["grp"] // PAIR, PAIR, sizes["fs"] // CORES, CORES, sizes["tp"])
    split = jax.sharding.Mesh(devices, ("pair", "member", "z", "core", "tp"))
    grp, fs = ("pair", "member"), ("z", "core")
    in_specs = (P((*grp, "tp"), None), P(fs), P(fs, "tp"), P(fs, "tp"))
    out_specs = (P(grp, fs), P(grp, fs), P((*grp, "tp"), fs))

    return jax.shard_map(local, mesh=split, in_specs=in_specs, out_specs=out_specs, check_vma=False)
```

```python
import functools

import jax
import jax.numpy as jnp
from jax import lax
from jax.experimental import pallas as pl
from jax.experimental.pallas import tpu as pltpu
from jax.sharding import PartitionSpec as P


epsilon = 1e-06
CORES = 2
PAIR = 2
LANES = 128


def ring(devices, step):
    return [(i, (i + step) % devices) for i in range(devices)]


def across(devices, step):
    return [
        (member * devices + i, (1 - member) * devices + (i + step) % devices)
        for member in range(PAIR)
        for i in range(devices)
    ]


def nt_dot(a, b):
    return lax.dot_general(a, b, (((1,), (1,)), ((), ())), preferred_element_type=jnp.float32)


def places(blocks, odd):
    return [(blocks - 1 - (3 if odd else 1) * block) % blocks for block in range(blocks)]


def partial_sums(out, parity, side, cores, active, down, parts=(1, 0)):
    shards, groups, quarter, width = down.shape
    rows, blocks = groups * quarter, shards // cores // 2
    head, tail = active[:LANES], active[LANES:]
    none = jnp.zeros_like(tail)
    upper, lower = jnp.concatenate([tail, none]), jnp.concatenate([none, tail])
    for at, part in enumerate(parts):
        at = part if len(parts) > 1 else at
        on = lax.rem(parity + part, 2) * cores + side
        weights = down.reshape(blocks, 2 * cores, rows, width)[:, pl.ds(on, 1)][:, 0]
        wide = nt_dot(weights.reshape(blocks * rows, width), head).astype(out.dtype).reshape(blocks, rows, LANES)
        packed = nt_dot(weights[:, : rows // 2].reshape(blocks * rows // 2, width), upper) + nt_dot(
            weights[:, rows // 2 :].reshape(blocks * rows // 2, width), lower
        )
        packed = packed.astype(out.dtype).reshape(blocks, rows // 2, LANES)
        odd = lax.rem(parity + part, 2)
        for block, (even_place, odd_place) in enumerate(zip(places(blocks, False), places(blocks, True))):
            place = pl.ds(jnp.where(odd == 0, even_place, odd_place), 1)
            out[at, place, :rows] = wide[block][None]
            out[at, place, rows:] = packed[block][None]


def feed_forward(cores, where, normed, *refs):
    quarters, (up, down, active, away) = refs[:-4], refs[-4:]
    shards, groups, quarter, width = up.shape
    at, core, member, parity = where[0], where[1], where[2], where[3]

    def place(weight, *pieces):
        for step, parts in enumerate(pieces):
            slot, first = lax.rem(at + step, groups), 0
            for part in parts:
                count = part.shape[0]
                weight[pl.ds(first, count), pl.ds(slot, 1)] = part[...][:, None]
                first += count

    own, left, far, right, twin, *rest, twin_right = quarters
    for value, mine, other in ((0, up, down), (1, down, up)):

        @pl.when(member == value)
        def _(mine=mine, other=other):
            place(mine, [own], [left], [far], [right])
            place(other, [twin], rest[:2], rest[2:], [twin_right])

    hidden = jnp.dot(
        normed[...], up[...].reshape(shards * groups * quarter, width), preferred_element_type=jnp.float32
    )
    rounded = jnp.square(jnp.maximum(hidden, 0.0)).astype(active.dtype)
    active[...] = rounded
    partial_sums(away, parity, 1 - core, cores, rounded, down)


def own_side(cores, where, active, up, down, up_out, down_out, kept, sems):
    writes = [pltpu.make_async_copy(up, up_out, sems.at[0]), pltpu.make_async_copy(down, down_out, sems.at[1])]
    for write in writes:
        write.start()
    partial_sums(kept, where[3], where[1], cores, active[...], down, (0,))
    for write in writes:
        write.wait()


def leaving_side(cores, where, active, down, kept):
    partial_sums(kept, where[3], where[1], cores, active[...], down, (1,))


def added(a, b):
    return (a.astype(jnp.float32) + b.astype(jnp.float32)).astype(jnp.bfloat16)


def summed_up(arrived, out):
    rows, cols = out.shape
    total = arrived[0].astype(jnp.float32)
    for chip in range(1, arrived.shape[0]):
        total += arrived[chip].astype(jnp.float32)
    total = total.astype(out.dtype)
    out[:, :LANES] = total[:rows]
    tail = total[rows:]
    out[: rows // 2, LANES:] = tail[:, : cols - LANES]
    out[rows // 2 :, LANES:] = tail[:, cols - LANES :]


def local(tokens, norm_gain, up_trained, down_trained):
    chips, cores, groups = lax.axis_size("z"), lax.axis_size("core"), lax.axis_size("tp")
    shards = chips * cores
    rows_local, cols_local = up_trained.shape
    count, features = tokens.shape
    width = cols_local * groups // shards
    blocks = cols_local // (width * cores)
    quarter = rows_local // groups
    where = jnp.stack([lax.axis_index("tp"), lax.axis_index("core"), lax.axis_index("member"), lax.axis_index("z") % 2]).astype(jnp.int32)
    smem, vmem = pl.BlockSpec(memory_space=pltpu.SMEM), pl.BlockSpec(memory_space=pltpu.VMEM)
    first = lax.axis_index("member") == 0
    mine = jnp.where(first, norm_gain[:, None] * up_trained, down_trained).astype(jnp.bfloat16)
    pieces = mine.reshape(groups, quarter, blocks, cores, width).transpose(3, 0, 2, 1, 4)
    pieces = pieces.reshape(cores * groups, blocks, quarter, width)
    moved = lax.all_to_all(pieces, ("core", "tp"), 0, 0, tiled=True)
    moved = moved.reshape(cores, chips, quarter, width).transpose(1, 0, 2, 3)
    own = lax.all_to_all(moved, "z", 0, 0, tiled=True).reshape(shards, quarter, width)
    values = tokens.astype(jnp.float32)
    scale = lax.rsqrt(jnp.mean(values * values, axis=1, keepdims=True) + epsilon)
    normed = (values * scale).astype(jnp.bfloat16)

    twin = lax.ppermute(own, "member", ring(PAIR, 1))
    left = lax.ppermute(own, "tp", ring(groups, -1))
    right = lax.ppermute(own, "tp", ring(groups, 1))
    cut, far_cut = shards // 2, shards // 4
    twin_right = lax.ppermute(twin, "tp", ring(groups, 1))
    far = lax.ppermute(left, "tp", ring(groups, -1))
    twin_left_first = lax.ppermute(left[:cut], "member", ring(PAIR, 1))
    twin_far_second = lax.ppermute(right[far_cut:], ("member", "tp"), across(groups, 1))
    twin_left_second = lax.ppermute(twin[cut:], "tp", ring(groups, -1))
    twin_far_first = lax.ppermute(left[:far_cut], ("member", "tp"), across(groups, -1))
    served = jax.ShapeDtypeStruct((shards, groups, quarter, width), jnp.bfloat16)
    part = jax.ShapeDtypeStruct((2, chips // 2, rows_local * count // LANES, LANES), jnp.bfloat16)
    up, down, active, away = pl.pallas_call(
        functools.partial(feed_forward, cores),
        out_shape=[served, served, jax.ShapeDtypeStruct((count, width), jnp.bfloat16), part],
        in_specs=[smem] + [vmem] * 11,
        out_specs=[vmem] * 4,
        compiler_params=pltpu.CompilerParams(vmem_limit_bytes=24 << 20),
        cost_estimate=pl.CostEstimate(
            flops=3 * count * features * width, bytes_accessed=8 * features * width, transcendentals=0
        ),
        name="feed_forward",
    )(
        where, normed, own, left, far, right,
        twin, twin_left_first, twin_left_second, twin_far_first, twin_far_second, twin_right,
    )
    one = jax.ShapeDtypeStruct((1, *part.shape[1:]), jnp.bfloat16)
    kept_leaving = pl.pallas_call(
        functools.partial(leaving_side, cores),
        out_shape=one,
        in_specs=[smem] + [vmem] * 2,
        out_specs=vmem,
        compiler_params=pltpu.CompilerParams(vmem_limit_bytes=16 << 20),
        cost_estimate=pl.CostEstimate(
            flops=count * features * width // 2, bytes_accessed=2 * features * width, transcendentals=0
        ),
        name="leaving_side",
    )(where, active, down)
    up_serving, down_serving, kept = pl.pallas_call(
        functools.partial(own_side, cores),
        out_shape=[served, served, one],
        in_specs=[smem] + [vmem] * 3,
        out_specs=[pl.BlockSpec(memory_space=pl.ANY)] * 2 + [vmem],
        scratch_shapes=[pltpu.SemaphoreType.DMA((2,))],
        compiler_params=pltpu.CompilerParams(vmem_limit_bytes=16 << 20),
        cost_estimate=pl.CostEstimate(
            flops=count * features * width, bytes_accessed=8 * features * width, transcendentals=0
        ),
        name="own_side",
    )(where, active, up, down)
    swapped = lax.ppermute(away, "core", ring(cores, 1))
    leaving = added(kept_leaving[0], swapped[1])
    mid = chips // 4
    up_one = lax.ppermute(leaving[:mid], "z", ring(chips, 1))
    down_one = lax.ppermute(leaving[mid:], "z", ring(chips, -1))
    summed = added(added(kept[0], swapped[0]), jnp.concatenate([up_one, down_one]))
    same_parity = [
        sorted(range(odd, chips, 2), key=lambda chip: places(chips // 2, odd)[chip // 2]) for odd in range(2)
    ]
    arrived = lax.all_to_all(summed, "z", 0, 0, axis_index_groups=same_parity, tiled=True)
    out = pl.pallas_call(
        summed_up,
        out_shape=jax.ShapeDtypeStruct((rows_local, count), jnp.bfloat16),
        in_specs=[vmem],
        out_specs=vmem,
        compiler_params=pltpu.CompilerParams(vmem_limit_bytes=8 << 20),
        name="summed_up",
    )(arrived).T
    return (up_serving.reshape(features, width), down_serving.reshape(features, width), out)


def solution(mesh):
    sizes = mesh.shape
    devices = mesh.devices.reshape(sizes["grp"] // PAIR, PAIR, sizes["fs"] // CORES, CORES, sizes["tp"])
    split = jax.sharding.Mesh(devices, ("pair", "member", "z", "core", "tp"))
    grp, fs = ("pair", "member"), ("z", "core")
    in_specs = (P((*grp, "tp"), None), P(fs), P(fs, "tp"), P(fs, "tp"))
    out_specs = (P(grp, fs), P(grp, fs), P((*grp, "tp"), fs))

    return jax.shard_map(local, mesh=split, in_specs=in_specs, out_specs=out_specs, check_vma=False)
```
